32 devices in a mesh: row: 16 (over z, y, x), col: 2 (over core).
Axes of the slice: x: 2, y: 2, z: 4, core: 2. Of those that a mesh axis runs over, the one named last changes fastest.
Arguments:
- tokens: bfloat16 [2, 6144, 2048], P('col', 'row'), may hold values from -6 to 6
- norm_gain: bfloat16 [2048], replicated, may hold values from 0.099609375 to 1.8984375
- in_weight: bfloat16 [2048, 512], P('row', 'col'), may hold values from -0.125 to 0.125
- out_weight: bfloat16 [512, 2048], P('col', 'row'), may hold values from -0.25 to 0.25
Outputs:
- mixed: bfloat16 [2, 6144, 2048], P('col', 'row')
The draws below stay inside these ranges and needn't reach their ends.
All inputs are finite; a program needn't handle non-finite values.
Results may differ from the reference program's by a relative error of at most 0.013.
Values may be sent and summed in bfloat16 or wider, within the bound.
A program may use at most 64 MiB of HBM per device.

```python
import jax
import jax.numpy as jnp
from jax import lax

D = 2048
FW = 512
GS = 64
GROUPS = 8
LEN = 6144
BATCH = 2


def block_scale(stream_key, extent, pieces, smallest, largest):
    def one(dim, parts):
        steps = jax.random.uniform(jax.random.fold_in(jax.random.fold_in(stream_key, 6), dim), (parts,), jnp.float32, smallest / len(pieces), largest / len(pieces))
        return jnp.repeat(jnp.exp(steps), extent[dim] // parts).reshape((-1,) + (1,) * (len(extent) - dim - 1))

    level = one(*pieces[0])
    for cut in pieces[1:]:
        level = level * one(*cut)
    return level


def bell_draw(key, extent, spread, limit, cuts=(), dtype=jnp.bfloat16):
    loudness = block_scale(key, extent, cuts, -0.22, 0.18) if cuts else 1.0
    values = jax.random.normal(key, extent, jnp.float32) * spread * loudness
    return jnp.minimum(jnp.maximum(values, -limit), limit).astype(dtype)


def setup_inputs(seed: int = 0) -> dict:
    streams_of = jax.random.split(jax.random.key(seed), 5)
    tokens = bell_draw(streams_of[0], (BATCH, LEN, D), 1.0, 6.0, ((0, 2), (1, 16)))
    norm_gain = jnp.clip(1.0 + 0.18 * jax.random.normal(streams_of[1], (D,), jnp.float32), 0.099609375, 1.8984375).astype(jnp.bfloat16)
    in_weight = bell_draw(streams_of[2], (D, FW), D ** -0.5, 0.125, ((0, 16), (1, 2)))
    out_weight = bell_draw(streams_of[3], (FW, D), FW ** -0.5, 0.25, ((0, 2), (1, 16)))
    return {"tokens": tokens, "norm_gain": norm_gain, "in_weight": in_weight, "out_weight": out_weight}


EPS = 1e-06

def mix_sequence(sequence, norm_gain, in_weight, out_weight):
    widened = sequence.astype(jnp.float32)
    inverse_rms = lax.rsqrt(lax.optimization_barrier(jnp.mean(widened * widened, axis=-1, keepdims=True)) + EPS)
    normed = (widened * inverse_rms * norm_gain.astype(jnp.float32)).astype(jnp.bfloat16)
    projected = jnp.dot(normed, in_weight, preferred_element_type=jnp.float32).astype(jnp.bfloat16)
    grouped = projected.astype(jnp.float32).reshape(LEN, GROUPS, GS)
    spectrum = jnp.fft.fftn(grouped, axes=(0, 2), norm='ortho')
    mixed_real = jnp.real(spectrum).reshape(LEN, FW).astype(jnp.bfloat16)
    return jnp.dot(mixed_real, out_weight, preferred_element_type=jnp.float32).astype(jnp.bfloat16)

def reference(tokens, norm_gain, in_weight, out_weight):
    return lax.map(lambda sequence: mix_sequence(sequence, norm_gain, in_weight, out_weight), tokens)
```

```python
import functools
import math

import jax
import jax.numpy as jnp
import numpy as np
from jax import lax
from jax.experimental import pallas as pl
from jax.experimental.pallas import tpu as pltpu
from jax.sharding import PartitionSpec as P

GS = 64
EPS = 1e-06
LANES = 128
F32 = jnp.float32
BF16 = jnp.bfloat16


def angles(left, right, modulus):
    product = np.arange(left)[:, None] * np.arange(right)[None, :] % modulus
    radians = product * (2.0 * math.pi / modulus)
    return np.cos(radians), np.sin(radians)


def channel_tables(narrow):
    cos, sin = angles(GS, GS, GS)
    half = narrow // 2
    forward = np.zeros((GS, GS))
    place_of = np.zeros((GS, GS))
    for slot in range(GS):
        owner, place = divmod(slot, narrow)
        j = owner * half + place % half
        if place < half:
            forward[slot] = cos[j]
            place_of[slot, j] = 1.0
        elif j == 0:
            forward[slot] = cos[GS // 2]
            place_of[slot, GS // 2] = 1.0
        else:
            forward[slot] = sin[j]
            place_of[slot, GS - j] = 1.0
    copies = np.eye(LANES // GS)
    return np.kron(copies, forward), np.kron(copies, place_of)


def tables(peers, rows, narrow):
    length = peers * rows
    forward, place_of = channel_tables(narrow)
    cos, sin = angles(peers, peers, peers)
    eye = np.eye(narrow)
    chunk = LANES // narrow
    first = np.concatenate(
        [
            np.kron(part[t : t + chunk], eye)
            for t in range(0, peers, chunk)
            for part in (cos, -sin)
        ]
    )
    turn = np.stack(angles(peers, rows, length)) / math.sqrt(length * GS)
    second = np.concatenate(angles(rows, rows, rows), axis=1)
    return (
        jnp.asarray(forward, BF16),
        jnp.asarray(place_of, BF16),
        jnp.asarray(first, BF16),
        jnp.asarray(turn, F32),
        jnp.asarray(second, BF16),
    )


def grid_of(peers):
    a = 2 if peers % 2 == 0 else 1
    b = 2 if peers // a % 2 == 0 else 1
    return peers // (a * b), b, a


def dot(a, b):
    return jnp.dot(a, b, preferred_element_type=F32)


def dot_nt(a, b):
    return lax.dot_general(a, b, (((1,), (1,)), ((), ())), preferred_element_type=F32)


def far_first(depth):
    return sorted(range(depth), key=lambda o: abs(2 * o - depth))


class Sems:
    def __init__(self, send, recv):
        self.send, self.recv, self.used = send, recv, 0

    def next(self):
        i = self.used
        self.used += 1
        assert i < self.send.shape[0]
        return self.send.at[i], self.recv.at[i]


def sem_count(peers, cols, gathers):
    depth, b, a = grid_of(peers)
    each = depth - 1 + (a - 1) + (b - 1) + cols - 1
    return gathers * each + 4 * (peers - 1)


def kernel(
    peers,
    cols,
    chunks,
    in_parts,
    out_parts,
    tokens_hbm,
    gain_hbm,
    in_hbm,
    out_w_hbm,
    forward_hbm,
    place_hbm,
    first_hbm,
    turn_hbm,
    second_hbm,
    mixed_ref,
    weight_ref,
    tokens,
    gain,
    forward,
    place_of,
    first,
    turn,
    second,
    normed,
    w_in,
    w_out,
    send_one,
    got_one,
    lines,
    send_two,
    got_two,
    arranged,
    load_sem,
    own_sem,
    send_sem,
    recv_sem,
):
    me = lax.axis_index("row")
    core = lax.axis_index("col")
    rows, width = tokens.shape
    depth, tall, wide = grid_of(peers)
    x = lax.rem(me, wide)
    y = lax.rem(lax.div(me, wide), tall)
    z = lax.div(me, wide * tall)
    block = w_in.shape[-1]
    span = cols * block
    narrow = span // peers
    half = narrow // 2
    step = rows // peers
    group = LANES // narrow
    sems = Sems(send_sem, recv_sem)

    def at_peer(dz, dy, dx):
        tz = lax.rem(z + dz, depth)
        ty = lax.rem(y + dy, tall)
        tx = lax.rem(x + dx, wide)
        return (tz * tall + ty) * wide + tx

    def mate(o):
        return lax.rem(core + o, cols)

    near = [(o, 0, 0) for o in range(1, depth)]
    near += [(0, o, 0) for o in range(1, tall)] + [(0, 0, o) for o in range(1, wide)]

    barrier = pltpu.get_barrier_semaphore()
    for o in near:
        pl.semaphore_signal(barrier, inc=1, device_id={"row": at_peer(*o)})
    for o in range(1, cols):
        pl.semaphore_signal(barrier, inc=1, device_id={"col": mate(o)})

    owns = [
        pltpu.make_async_copy(
            in_hbm.at[:, c * block : (c + 1) * block], w_in.at[c, core, z, y, x], own_sem.at[c]
        )
        for c in range(chunks)
    ]
    owns.append(pltpu.make_async_copy(out_w_hbm, w_out.at[core, z, y, x], own_sem.at[chunks]))
    loads = [
        pltpu.make_async_copy(src, dst, load_sem.at[i])
        for i, (src, dst) in enumerate(
            (
                (tokens_hbm, tokens),
                (gain_hbm, gain),
                (forward_hbm, forward),
                (place_hbm, place_of),
                (first_hbm, first),
                (turn_hbm, turn),
                (second_hbm, second),
            )
        )
    ]
    for load in owns[:chunks] + loads[:2] + owns[chunks:] + loads[2:]:
        load.start()
    for own in owns[:chunks]:
        own.wait()
    pl.semaphore_wait(barrier, len(near) + cols - 1)

    sent = []

    def remote(src, dst, device):
        send, recv = sems.next()
        copy = pltpu.make_async_remote_copy(
            src_ref=src, dst_ref=dst, send_sem=send, recv_sem=recv, device_id=device
        )
        copy.start()
        sent.append(copy)
        return copy

    class Part:
        def __init__(self, buffer, index, height):
            self.buffer, self.at, self.flip = buffer, pl.ds(index * height, height), index % 2
            self.stage, self.open = 0, []

        def push(self):
            for copy in self.open:
                copy.wait_recv()
            held, everything = self.buffer.at[core], slice(None)
            if self.stage == 0:
                targets = [
                    (held.at[z, y, x, self.at], {"row": at_peer(o, 0, 0)})
                    for o in far_first(depth)
                    if o
                ]
            elif self.stage == 3:
                targets = [
                    (held.at[:, :, :, self.at], {"col": mate(o)}) for o in range(1, cols)
                ]
            else:
                along_x = (self.stage == 1) != bool(self.flip)
                if self.stage == 1:
                    ref = held.at[:, y, x, self.at]
                elif along_x:
                    ref = held.at[:, :, x, self.at]
                else:
                    ref = held.at[:, y, :, self.at]
                extent = wide if along_x else tall
                targets = [
                    (ref, {"row": at_peer(0, 0, o) if along_x else at_peer(0, o, 0)})
                    for o in range(1, extent)
                ]
            self.open = [remote(ref, ref, device) for ref, device in targets]
            self.stage += 1

        def finish(self):
            for copy in self.open:
                copy.wait_recv()

    def parts_of(buffer, count):
        height = buffer.shape[-2] // count
        return [Part(buffer, i, height) for i in range(count)]

    gather_in = [parts_of(w_in.at[c], in_parts) for c in range(chunks)]
    gather_out = parts_of(w_out, out_parts)
    def push(parts):
        for part in parts:
            part.push()

    push(gather_in[0])

    loads[0].wait()
    loads[1].wait()
    scale = gain[...].astype(F32).reshape(1, width)
    tile = 32

    def norm(i, carry):
        at = pl.ds(pl.multiple_of(i * tile, tile), tile)
        rows_of = tokens[at, :].astype(F32)
        inverse = lax.rsqrt(jnp.mean(rows_of * rows_of, axis=-1, keepdims=True) + EPS)
        normed[at, :] = (rows_of * inverse * scale).astype(BF16)
        return carry

    lax.fori_loop(0, rows // tile, norm, 0)

    push(gather_in[0])
    for c in range(1, chunks):
        push(gather_in[c])
    push(gather_in[0])
    for c in range(1, chunks):
        push(gather_in[c])
    owns[chunks].wait()
    push(gather_out)
    push(gather_in[0])
    for c in range(1, chunks):
        push(gather_in[c])
    for load in loads[2:]:
        load.wait()

    flights = {}

    def exchange(which, c, src, dst):
        copies = []
        for dz in far_first(depth):
            for dy in reversed(range(tall)):
                for dx in reversed(range(wide)):
                    if dz or dy or dx:
                        to = at_peer(dz, dy, dx)
                        copies.append(remote(src.at[to], dst.at[me], {"row": to}))
        own = pltpu.make_async_copy(src.at[me], dst.at[me], own_sem.at[chunks + 1])
        own.start()
        own.wait()
        flights[which, c] = copies

    def land(which, c):
        for copy in flights[which, c]:
            copy.wait_recv()

    def project(c):
        weight = jnp.concatenate(
            [w_in[c, i].reshape(width, block) for i in range(cols)], axis=1
        )
        projected = dot(normed[...], weight).astype(BF16)
        for b in range(0, span, LANES):
            slots = dot_nt(forward[...], projected[:, b : b + LANES]).astype(BF16)
            send_one[c, b // narrow : (b + LANES) // narrow] = slots.reshape(
                group, narrow, rows
            )

    leads = lax.rem(me * narrow, GS) == 0
    alone = (lax.broadcasted_iota(jnp.int32, (half, rows), 0) == 0) & leads

    def transform(c):
        columns = got_one[c].reshape(span, rows)
        for t0 in range(0, peers, group):
            both = dot(first[2 * t0 * narrow : 2 * (t0 + group) * narrow, :], columns)
            for i in range(group):
                t = t0 + i
                real = both[i * narrow : (i + 1) * narrow]
                imag = both[LANES + i * narrow : LANES + (i + 1) * narrow]
                cos = turn[0, t : t + 1, :]
                sin = turn[1, t : t + 1, :]
                z_real = real * cos + imag * sin
                z_imag = imag * cos - real * sin
                c_real, s_real = z_real[:half], z_real[half:]
                c_imag, s_imag = z_imag[:half], z_imag[half:]
                low = slice(t * narrow, t * narrow + half)
                high = slice(t * narrow + half, (t + 1) * narrow)
                lines[low, :rows] = jnp.where(alone, c_real, c_real + s_imag)
                lines[low, rows:] = jnp.where(alone, c_imag, c_imag - s_real)
                lines[high, :rows] = jnp.where(alone, s_real, c_real - s_imag)
                lines[high, rows:] = jnp.where(alone, s_imag, c_imag + s_real)
        whole = dot_nt(second[...], lines[...].astype(BF16))
        send_two[c] = whole.reshape(peers, step, span).astype(BF16)

    lane_block = lax.broadcasted_iota(jnp.int32, (step, LANES), 1) // narrow

    def arrange(c):
        for d0 in range(0, peers, group):
            for t0 in range(0, peers, group):
                held = [
                    got_two[c, d0 + i, :, t0 * narrow : (t0 + group) * narrow].astype(F32)
                    for i in range(group)
                ]
                stride = group // 2
                while stride:
                    upper = (lane_block // stride) % 2 == 1
                    for i in range(group):
                        if i // stride % 2 == 0:
                            a, b = held[i], held[i + stride]
                            held[i] = jnp.where(upper, pltpu.roll(b, stride * narrow, 1), a)
                            held[i + stride] = jnp.where(
                                upper, b, pltpu.roll(a, LANES - stride * narrow, 1)
                            )
                    stride //= 2
                for j in range(group):
                    arranged[d0 // group, pl.ds(t0 + j, step, stride=peers), :] = held[j]
        for b in range(0, span, LANES):
            at = c * span + b
            mixed_ref[:, at : at + LANES] = arranged[b // LANES].astype(BF16)

    def weigh():
        for c in range(chunks):
            for i in range(cols):
                for b in range(0, block, LANES):
                    high = min(LANES, block)
                    w = w_out[i, :, :, :, c * block + b : c * block + b + high, :]
                    w = w.reshape(peers, high, w.shape[-1])
                    w = jnp.concatenate([w[p] for p in range(peers)], axis=1)
                    at = c * span + i * block + b
                    weight_ref[at : at + high, :] = dot(place_of[:high, :high], w).astype(BF16)

    for c in range(chunks):
        if c:
            push(gather_in[c])
        for part in gather_in[c]:
            part.finish()
        project(c)
        exchange(0, c, send_one.at[c], got_one.at[c])
        if c == 0:
            push(gather_out)

    push(gather_out[: len(gather_out) // 2])
    for c in range(chunks):
        land(0, c)
        transform(c)
        exchange(1, c, send_two.at[c], got_two.at[c])
        if c == 0:
            push(gather_out[len(gather_out) // 2 :])
    push(gather_out)
    last = flights[1, chunks - 1]
    for c in range(chunks):
        land(1, c) if c + 1 < chunks else None
        if c + 1 < chunks:
            arrange(c)
    for part in gather_out:
        part.finish()
    weigh()
    late = {id(copy) for copy in last}
    for copy in sent:
        if id(copy) not in late:
            copy.wait_send()
    land(1, chunks - 1)
    arrange(chunks - 1)
    for copy in last:
        copy.wait_send()


def close(mixed_ref, weight_ref, result_ref, result, store_sem):
    width = result.shape[1]
    piece = min(256, width)
    stores = []
    for i in range(width // piece):
        at = slice(i * piece, (i + 1) * piece)
        result[:, at] = dot(mixed_ref[...], weight_ref[:, at]).astype(BF16)
        store = pltpu.make_async_copy(result.at[:, at], result_ref.at[:, at], store_sem.at[i])
        store.start()
        stores.append(store)
    for store in stores:
        store.wait()


def body(peers, cols, tokens, norm_gain, in_weight, out_weight):
    rows, width = tokens.shape[1:]
    in_rows, in_cols = in_weight.shape
    out_rows, out_cols = out_weight.shape
    channels = in_cols * cols
    depth, tall, wide = grid_of(peers)
    chunks = 2 if in_cols % (2 * LANES) == 0 else 1
    block = in_cols // chunks
    span = block * cols
    narrow = span // peers
    step = rows // peers
    in_parts = max(1, min(4, in_rows // 16))
    out_parts = max(1, min(4, out_rows // 16))
    forward, place_of, first, turn, second = tables(peers, rows, narrow)
    vmem = pl.BlockSpec(memory_space=pltpu.VMEM)
    hbm = pl.BlockSpec(memory_space=pltpu.HBM)
    count = sem_count(peers, cols, chunks * in_parts + out_parts)
    mixed, weight = pl.pallas_call(
        functools.partial(kernel, peers, cols, chunks, in_parts, out_parts),
        out_shape=(
            pltpu.VMEM((rows, channels), BF16),
            pltpu.VMEM((channels, width), BF16),
        ),
        in_specs=[hbm] * 9,
        out_specs=(vmem, vmem),
        scratch_shapes=[
            pltpu.VMEM((rows, width), BF16),
            pltpu.VMEM((width,), BF16),
            pltpu.VMEM(forward.shape, BF16),
            pltpu.VMEM(place_of.shape, BF16),
            pltpu.VMEM(first.shape, BF16),
            pltpu.VMEM(turn.shape, F32),
            pltpu.VMEM(second.shape, BF16),
            pltpu.VMEM((rows, width), BF16),
            pltpu.VMEM((chunks, cols, depth, tall, wide, in_rows, block), BF16),
            pltpu.VMEM((cols, depth, tall, wide, out_rows, out_cols), BF16),
            pltpu.VMEM((chunks, peers, narrow, rows), BF16),
            pltpu.VMEM((chunks, peers, narrow, rows), BF16),
            pltpu.VMEM((span, 2 * rows), F32),
            pltpu.VMEM((chunks, peers, step, span), BF16),
            pltpu.VMEM((chunks, peers, step, span), BF16),
            pltpu.VMEM((span // LANES, rows, LANES), F32),
            pltpu.SemaphoreType.DMA((7,)),
            pltpu.SemaphoreType.DMA((chunks + 2,)),
            pltpu.SemaphoreType.DMA((count,)),
            pltpu.SemaphoreType.DMA((count,)),
        ],
        compiler_params=pltpu.CompilerParams(
            collective_id=0, has_side_effects=True, vmem_limit_bytes=32 * 1024 * 1024
        ),
    )(
        *(
            pltpu.with_memory_space_constraint(a, pltpu.HBM)
            for a in (
                tokens[0],
                norm_gain,
                in_weight,
                out_weight,
                forward,
                place_of,
                first,
                turn,
                second,
            )
        )
    )
    pieces = width // min(256, width)
    result = pl.pallas_call(
        close,
        out_shape=jax.ShapeDtypeStruct((rows, width), BF16),
        in_specs=[vmem, vmem],
        out_specs=hbm,
        scratch_shapes=[
            pltpu.VMEM((rows, width), BF16),
            pltpu.SemaphoreType.DMA((pieces,)),
        ],
        compiler_params=pltpu.CompilerParams(vmem_limit_bytes=16 * 1024 * 1024),
    )(mixed, weight)
    return result[None]


def solution(mesh):
    in_specs = (P("col", "row", None), P(), P("row", "col"), P("col", "row"))
    out_specs = P("col", "row", None)
    step = functools.partial(body, mesh.shape["row"], mesh.shape["col"])
    return jax.shard_map(step, mesh=mesh, in_specs=in_specs, out_specs=out_specs, check_vma=False)
```

```python
import functools
import math

import jax
import jax.numpy as jnp
import numpy as np
from jax import lax
from jax.experimental import pallas as pl
from jax.experimental.pallas import tpu as pltpu
from jax.sharding import PartitionSpec as P

GS = 64
EPS = 1e-06
LANES = 128
F32 = jnp.float32
BF16 = jnp.bfloat16


def angles(left, right, modulus):
    product = np.arange(left)[:, None] * np.arange(right)[None, :] % modulus
    radians = product * (2.0 * math.pi / modulus)
    return np.cos(radians), np.sin(radians)


def channel_tables(narrow):
    cos, sin = angles(GS, GS, GS)
    half = narrow // 2
    forward = np.zeros((GS, GS))
    place_of = np.zeros((GS, GS))
    for slot in range(GS):
        owner, place = divmod(slot, narrow)
        j = owner * half + place % half
        if place < half:
            forward[slot] = cos[j]
            place_of[slot, j] = 1.0
        elif j == 0:
            forward[slot] = cos[GS // 2]
            place_of[slot, GS // 2] = 1.0
        else:
            forward[slot] = sin[j]
            place_of[slot, GS - j] = 1.0
    copies = np.eye(LANES // GS)
    return np.kron(copies, forward), np.kron(copies, place_of)


def tables(peers, rows, narrow):
    length = peers * rows
    forward, place_of = channel_tables(narrow)
    cos, sin = angles(peers, peers, peers)
    eye = np.eye(narrow)
    chunk = LANES // narrow
    first = np.concatenate(
        [
            np.kron(part[t : t + chunk], eye)
            for t in range(0, peers, chunk)
            for part in (cos, -sin)
        ]
    )
    turn = np.stack(angles(peers, rows, length)) / math.sqrt(length * GS)
    second = np.concatenate(angles(rows, rows, rows), axis=1)
    return (
        jnp.asarray(forward, BF16),
        jnp.asarray(place_of, BF16),
        jnp.asarray(first, BF16),
        jnp.asarray(turn, F32),
        jnp.asarray(second, BF16),
    )


def grid_of(peers):
    a = 2 if peers % 2 == 0 else 1
    b = 2 if peers // a % 2 == 0 else 1
    return peers // (a * b), b, a


def dot(a, b):
    return jnp.dot(a, b, preferred_element_type=F32)


def dot_nt(a, b):
    return lax.dot_general(a, b, (((1,), (1,)), ((), ())), preferred_element_type=F32)


def far_first(depth):
    return sorted(range(depth), key=lambda o: abs(2 * o - depth))


def kernel(
    peers,
    cols,
    chunks,
    in_parts,
    out_parts,
    tokens_hbm,
    gain_hbm,
    in_hbm,
    out_w_hbm,
    forward_hbm,
    place_hbm,
    first_hbm,
    turn_hbm,
    second_hbm,
    mixed_ref,
    weight_ref,
    tokens,
    gain,
    forward,
    place_of,
    first,
    turn,
    second,
    normed,
    w_in,
    w_out,
    send_one,
    got_one,
    lines,
    send_two,
    got_two,
    arranged,
    load_sem,
    own_sem,
    flow_send,
    flow_recv,
    swap_send,
    swap_recv,
):
    me = lax.axis_index("row")
    core = lax.axis_index("col")
    rows, width = tokens.shape
    depth, tall, wide = grid_of(peers)
    x = lax.rem(me, wide)
    y = lax.rem(lax.div(me, wide), tall)
    z = lax.div(me, wide * tall)
    block = w_in.shape[-1]
    span = cols * block
    narrow = span // peers
    half = narrow // 2
    step = rows // peers
    group = LANES // narrow

    def at_peer(dz, dy, dx):
        tz = lax.rem(z + dz, depth)
        ty = lax.rem(y + dy, tall)
        tx = lax.rem(x + dx, wide)
        return (tz * tall + ty) * wide + tx

    def mate(o):
        return lax.rem(core + o, cols)

    near = [(o, 0, 0) for o in range(1, depth)]
    near += [(0, o, 0) for o in range(1, tall)] + [(0, 0, o) for o in range(1, wide)]

    barrier = pltpu.get_barrier_semaphore()
    for o in near:
        pl.semaphore_signal(barrier, inc=1, device_id={"row": at_peer(*o)})
    for o in range(1, cols):
        pl.semaphore_signal(barrier, inc=1, device_id={"col": mate(o)})

    owns = [
        pltpu.make_async_copy(
            in_hbm.at[:, c * block : (c + 1) * block], w_in.at[c, core, z, y, x], own_sem.at[c]
        )
        for c in range(chunks)
    ]
    owns.append(pltpu.make_async_copy(out_w_hbm, w_out.at[core, z, y, x], own_sem.at[chunks]))
    loads = [
        pltpu.make_async_copy(src, dst, load_sem.at[i])
        for i, (src, dst) in enumerate(
            (
                (tokens_hbm, tokens),
                (gain_hbm, gain),
                (forward_hbm, forward),
                (place_hbm, place_of),
                (first_hbm, first),
                (turn_hbm, turn),
                (second_hbm, second),
            )
        )
    ]
    for load in owns[:chunks] + loads[:2] + owns[chunks:] + loads[2:]:
        load.start()
    for own in owns[:chunks]:
        own.wait()
    pl.semaphore_wait(barrier, len(near) + cols - 1)

    def remote(src, dst, send, recv, device):
        pltpu.make_async_remote_copy(
            src_ref=src, dst_ref=dst, send_sem=send, recv_sem=recv, device_id=device
        ).start()

    def settle(ref, sem):
        pltpu.make_async_copy(ref, ref, sem).wait()

    class Part:
        def __init__(self, which, index, buffer, height):
            self.which, self.index, self.buffer = which, index, buffer
            self.at, self.flip = pl.ds(index * height, height), index % 2
            self.stage = 0

        def along_x(self, stage):
            return (stage == 1) != bool(self.flip)

        def extent(self, stage):
            if stage in (0, 3):
                return cols if stage else depth
            return wide if self.along_x(stage) else tall

        def amount(self, stage, at):
            held = self.buffer.at[core]
            if stage == 0:
                return held.at[pl.ds(0, depth - 1), 0, 0, at]
            if stage == 3:
                return self.buffer.at[pl.ds(0, cols - 1), :, :, :, at]
            if stage == 1:
                return held.at[:, 0, 0, at]
            return held.at[:, :, 0, at] if self.along_x(stage) else held.at[:, 0, :, at]

        def land(self):
            if self.stage and self.extent(self.stage - 1) > 1:
                settle(
                    self.amount(self.stage - 1, self.at),
                    flow_recv.at[self.which, self.stage - 1, self.index],
                )

        def push(self):
            self.land()
            held, stage = self.buffer.at[core], self.stage
            if stage == 0:
                ref = held.at[z, y, x, self.at]
                targets = [{"row": at_peer(o, 0, 0)} for o in far_first(depth) if o]
            elif stage == 3:
                ref = held.at[:, :, :, self.at]
                targets = [{"col": mate(o)} for o in range(1, cols)]
            else:
                along_x = self.along_x(stage)
                if stage == 1:
                    ref = held.at[:, y, x, self.at]
                elif along_x:
                    ref = held.at[:, :, x, self.at]
                else:
                    ref = held.at[:, y, :, self.at]
                targets = [
                    {"row": at_peer(0, 0, o) if along_x else at_peer(0, o, 0)}
                    for o in range(1, self.extent(stage))
                ]
            for device in targets:
                send = flow_send.at[self.which, stage, self.index % 2]
                recv = flow_recv.at[self.which, stage, self.index]
                remote(ref, ref, send, recv, device)
            self.stage += 1

    def parts_of(which, buffer, count):
        height = buffer.shape[-2] // count
        return [Part(which, i, buffer, height) for i in range(count)]

    gather_in = [parts_of(c, w_in.at[c], in_parts) for c in range(chunks)]
    gather_out = parts_of(chunks, w_out, out_parts)

    def drain(parts):
        for stage in range(4):
            for side in range(min(2, len(parts))):
                some = parts[side::2]
                if some[0].extent(stage) > 1:
                    settle(
                        some[0].amount(stage, pl.ds(0, some[0].at.size * len(some))),
                        flow_send.at[some[0].which, stage, side],
                    )

    def push(parts):
        for part in parts:
            part.push()

    push(gather_in[0])

    loads[0].wait()
    loads[1].wait()
    scale = gain[...].astype(F32).reshape(1, width)
    tile = 32

    def norm(i, carry):
        at = pl.ds(pl.multiple_of(i * tile, tile), tile)
        rows_of = tokens[at, :].astype(F32)
        inverse = lax.rsqrt(jnp.mean(rows_of * rows_of, axis=-1, keepdims=True) + EPS)
        normed[at, :] = (rows_of * inverse * scale).astype(BF16)
        return carry

    lax.fori_loop(0, rows // tile, norm, 0)

    push(gather_in[0])
    for c in range(1, chunks):
        push(gather_in[c])
    push(gather_in[0])
    for c in range(1, chunks):
        push(gather_in[c])
    owns[chunks].wait()
    push(gather_out)
    push(gather_in[0])
    for c in range(1, chunks):
        push(gather_in[c])
    for load in loads[2:]:
        load.wait()

    def exchange(which, c, src, dst):
        for dz in far_first(depth):
            for dy in reversed(range(tall)):
                for dx in reversed(range(wide)):
                    if dz or dy or dx:
                        to = at_peer(dz, dy, dx)
                        send, recv = swap_send.at[which, c], swap_recv.at[which, c]
                        remote(src.at[to], dst.at[me], send, recv, {"row": to})
        own = pltpu.make_async_copy(src.at[me], dst.at[me], own_sem.at[chunks + 1])
        own.start()
        own.wait()

    others = pl.ds(0, peers - 1)

    def land(dst, which, c):
        settle(dst.at[c, others], swap_recv.at[which, c])

    def project(c):
        weight = jnp.concatenate(
            [w_in[c, i].reshape(width, block) for i in range(cols)], axis=1
        )
        projected = dot(normed[...], weight).astype(BF16)
        for b in range(0, span, LANES):
            slots = dot_nt(forward[...], projected[:, b : b + LANES]).astype(BF16)
            send_one[c, b // narrow : (b + LANES) // narrow] = slots.reshape(
                group, narrow, rows
            )

    leads = lax.rem(me * narrow, GS) == 0
    alone = (lax.broadcasted_iota(jnp.int32, (half, rows), 0) == 0) & leads

    def transform(c):
        columns = got_one[c].reshape(span, rows)
        for t0 in range(0, peers, group):
            both = dot(first[2 * t0 * narrow : 2 * (t0 + group) * narrow, :], columns)
            for i in range(group):
                t = t0 + i
                real = both[i * narrow : (i + 1) * narrow]
                imag = both[LANES + i * narrow : LANES + (i + 1) * narrow]
                cos = turn[0, t : t + 1, :]
                sin = turn[1, t : t + 1, :]
                z_real = real * cos + imag * sin
                z_imag = imag * cos - real * sin
                c_real, s_real = z_real[:half], z_real[half:]
                c_imag, s_imag = z_imag[:half], z_imag[half:]
                low = slice(t * narrow, t * narrow + half)
                high = slice(t * narrow + half, (t + 1) * narrow)
                lines[low, :rows] = jnp.where(alone, c_real, c_real + s_imag)
                lines[low, rows:] = jnp.where(alone, c_imag, c_imag - s_real)
                lines[high, :rows] = jnp.where(alone, s_real, c_real - s_imag)
                lines[high, rows:] = jnp.where(alone, s_imag, c_imag + s_real)
        whole = dot_nt(second[...], lines[...].astype(BF16))
        send_two[c] = whole.reshape(peers, step, span).astype(BF16)

    lane_block = lax.broadcasted_iota(jnp.int32, (step, LANES), 1) // narrow

    def arrange(c):
        for d0 in range(0, peers, group):
            for t0 in range(0, peers, group):
                held = [
                    got_two[c, d0 + i, :, t0 * narrow : (t0 + group) * narrow].astype(F32)
                    for i in range(group)
                ]
                stride = group // 2
                while stride:
                    upper = (lane_block // stride) % 2 == 1
                    for i in range(group):
                        if i // stride % 2 == 0:
                            a, b = held[i], held[i + stride]
                            held[i] = jnp.where(upper, pltpu.roll(b, stride * narrow, 1), a)
                            held[i + stride] = jnp.where(
                                upper, b, pltpu.roll(a, LANES - stride * narrow, 1)
                            )
                    stride //= 2
                for j in range(group):
                    arranged[d0 // group, pl.ds(t0 + j, step, stride=peers), :] = held[j]
        for b in range(0, span, LANES):
            at = c * span + b
            mixed_ref[:, at : at + LANES] = arranged[b // LANES].astype(BF16)

    def weigh():
        for c in range(chunks):
            for i in range(cols):
                for b in range(0, block, LANES):
                    high = min(LANES, block)
                    w = w_out[i, :, :, :, c * block + b : c * block + b + high, :]
                    w = w.reshape(peers, high, w.shape[-1])
                    w = jnp.concatenate([w[p] for p in range(peers)], axis=1)
                    at = c * span + i * block + b
                    weight_ref[at : at + high, :] = dot(place_of[:high, :high], w).astype(BF16)

    for c in range(chunks):
        if c:
            push(gather_in[c])
        for part in gather_in[c]:
            part.land()
        project(c)
        exchange(0, c, send_one.at[c], got_one.at[c])
        if c == 0:
            push(gather_out)

    push(gather_out[: len(gather_out) // 2])
    for c in range(chunks):
        land(got_one, 0, c)
        transform(c)
        exchange(1, c, send_two.at[c], got_two.at[c])
        if c == 0:
            push(gather_out[len(gather_out) // 2 :])
    push(gather_out)
    for c in range(chunks - 1):
        land(got_two, 1, c)
        arrange(c)
    for part in gather_out:
        part.land()
    weigh()
    for parts in gather_in + [gather_out]:
        drain(parts)
    for c in range(chunks):
        settle(send_one.at[c, others], swap_send.at[0, c])
    land(got_two, 1, chunks - 1)
    arrange(chunks - 1)
    for c in range(chunks):
        settle(send_two.at[c, others], swap_send.at[1, c])


def close(mixed_ref, weight_ref, result_ref, result, store_sem):
    width = result.shape[1]
    piece = min(256, width)
    stores = []
    for i in range(width // piece):
        at = slice(i * piece, (i + 1) * piece)
        result[:, at] = dot(mixed_ref[...], weight_ref[:, at]).astype(BF16)
        store = pltpu.make_async_copy(result.at[:, at], result_ref.at[:, at], store_sem.at[i])
        store.start()
        stores.append(store)
    for store in stores:
        store.wait()


def body(peers, cols, tokens, norm_gain, in_weight, out_weight):
    rows, width = tokens.shape[1:]
    in_rows, in_cols = in_weight.shape
    out_rows, out_cols = out_weight.shape
    channels = in_cols * cols
    depth, tall, wide = grid_of(peers)
    chunks = 2 if in_cols % (2 * LANES) == 0 else 1
    block = in_cols // chunks
    span = block * cols
    narrow = span // peers
    step = rows // peers
    in_parts = max(1, min(4, in_rows // 16))
    out_parts = max(1, min(4, out_rows // 16))
    forward, place_of, first, turn, second = tables(peers, rows, narrow)
    vmem = pl.BlockSpec(memory_space=pltpu.VMEM)
    hbm = pl.BlockSpec(memory_space=pltpu.HBM)
    mixed, weight = pl.pallas_call(
        functools.partial(kernel, peers, cols, chunks, in_parts, out_parts),
        out_shape=(
            pltpu.VMEM((rows, channels), BF16),
            pltpu.VMEM((channels, width), BF16),
        ),
        in_specs=[hbm] * 9,
        out_specs=(vmem, vmem),
        scratch_shapes=[
            pltpu.VMEM((rows, width), BF16),
            pltpu.VMEM((width,), BF16),
            pltpu.VMEM(forward.shape, BF16),
            pltpu.VMEM(place_of.shape, BF16),
            pltpu.VMEM(first.shape, BF16),
            pltpu.VMEM(turn.shape, F32),
            pltpu.VMEM(second.shape, BF16),
            pltpu.VMEM((rows, width), BF16),
            pltpu.VMEM((chunks, cols, depth, tall, wide, in_rows, block), BF16),
            pltpu.VMEM((cols, depth, tall, wide, out_rows, out_cols), BF16),
            pltpu.VMEM((chunks, peers, narrow, rows), BF16),
            pltpu.VMEM((chunks, peers, narrow, rows), BF16),
            pltpu.VMEM((span, 2 * rows), F32),
            pltpu.VMEM((chunks, peers, step, span), BF16),
            pltpu.VMEM((chunks, peers, step, span), BF16),
            pltpu.VMEM((span // LANES, rows, LANES), F32),
            pltpu.SemaphoreType.DMA((7,)),
            pltpu.SemaphoreType.DMA((chunks + 2,)),
            pltpu.SemaphoreType.DMA((chunks + 1, 4, 2)),
            pltpu.SemaphoreType.DMA((chunks + 1, 4, max(in_parts, out_parts))),
            pltpu.SemaphoreType.DMA((2, chunks)),
            pltpu.SemaphoreType.DMA((2, chunks)),
        ],
        compiler_params=pltpu.CompilerParams(
            collective_id=0, has_side_effects=True, vmem_limit_bytes=32 * 1024 * 1024
        ),
    )(
        *(
            pltpu.with_memory_space_constraint(a, pltpu.HBM)
            for a in (
                tokens[0],
                norm_gain,
                in_weight,
                out_weight,
                forward,
                place_of,
                first,
                turn,
                second,
            )
        )
    )
    pieces = width // min(256, width)
    result = pl.pallas_call(
        close,
        out_shape=jax.ShapeDtypeStruct((rows, width), BF16),
        in_specs=[vmem, vmem],
        out_specs=hbm,
        scratch_shapes=[
            pltpu.VMEM((rows, width), BF16),
            pltpu.SemaphoreType.DMA((pieces,)),
        ],
        compiler_params=pltpu.CompilerParams(vmem_limit_bytes=16 * 1024 * 1024),
    )(mixed, weight)
    return result[None]


def solution(mesh):
    in_specs = (P("col", "row", None), P(), P("row", "col"), P("col", "row"))
    out_specs = P("col", "row", None)
    step = functools.partial(body, mesh.shape["row"], mesh.shape["col"])
    return jax.shard_map(step, mesh=mesh, in_specs=in_specs, out_specs=out_specs, check_vma=False)
```
